512 devices in a mesh: fs: 128 (over z, x, core), tp: 4 (over y).
Axes of the slice: x: 4, y: 4, z: 16, core: 2. Of those that a mesh axis runs over, the one named last changes fastest.
Arguments:
- tokens: bfloat16 [16384, 2048], P('fs'), may hold values from -6 to 6
- gain: float32 [2048], P('fs'), may hold values from 0.1 to 1.9
- up_master: float32 [2048, 8192], P('fs', 'tp'), may hold values from -0.125 to 0.125
- down_master: float32 [2048, 8192], P('fs', 'tp'), may hold values from -0.0625 to 0.0625
Outputs:
- up_sampled: bfloat16 [128, 2048, 1024], P('fs', None, 'tp')
- down_sampled: bfloat16 [128, 2048, 1024], P('fs', None, 'tp')
- mixed: bfloat16 [16384, 2048], P('fs', 'tp')
The draws below stay inside these ranges and needn't reach their ends.
All inputs are finite; a program needn't handle non-finite values.
Results may differ from the reference program's by a relative error of at most 0.0087.
Values may be sent and summed in bfloat16 or wider, within the bound.
No kernel may reach another device: no remote copies, remote signals or barrier semaphores. Data moves between devices by JAX's collectives and lax.ppermute only.
A program may use at most 64 MiB of HBM per device.

```python
import jax
import jax.numpy as jnp
from jax import lax

D = 2048
FF = 8192
SUB = 8
TOKENS = 16384
UNITS_DEV = 256
N_FS = 128
N_TP = 4


def levels(stream_key, shape, split, smallest, largest):
    def one(axis_at, shards_of):
        draws = jax.random.uniform(jax.random.fold_in(jax.random.fold_in(stream_key, 6), axis_at), (shards_of,), jnp.float32, smallest / len(split), largest / len(split))
        return jnp.repeat(jnp.exp(draws), shape[axis_at] // shards_of).reshape((-1,) + (1,) * (len(shape) - axis_at - 1))

    level = one(*split[0])
    for cut in split[1:]:
        level = level * one(*cut)
    return level


def centred(stream_key, shape, width, bound, split=(), kind=jnp.bfloat16):
    drawn = width * jax.random.normal(stream_key, shape, jnp.float32)
    if split:
        drawn = drawn * levels(stream_key, shape, split, -0.22, 0.18)
    return jnp.clip(drawn, -bound, bound).astype(kind)


def setup_inputs(seed: int = 0) -> dict:
    key_list = jax.random.split(jax.random.key(seed), 5)
    tokens = centred(key_list[0], (TOKENS, D), 1.0, 6.0, ((0, 128),))
    gain = jnp.clip(1.0 + 0.18 * jax.random.normal(key_list[1], (D,), jnp.float32), 0.1, 1.9)
    up_master = centred(key_list[2], (D, FF), D ** -0.5, 0.125, ((0, 128), (1, 4)), jnp.float32)
    down_master = centred(key_list[3], (D, FF), FF ** -0.5, 0.0625, ((0, 128), (1, 4)), jnp.float32)
    return dict(tokens=tokens, gain=gain, up_master=up_master, down_master=down_master)


def sampled(weight):
    blocks = weight.reshape(D, N_TP, SUB, UNITS_DEV).transpose(2, 0, 1, 3).reshape(SUB, D, N_TP * UNITS_DEV)
    return jnp.tile(blocks, (N_FS // SUB, 1, 1))

def reference(tokens, gain, up_master, down_master):
    up_round = (gain[:, None] * up_master).astype(jnp.bfloat16)
    down_round = down_master.astype(jnp.bfloat16)
    widened = tokens.astype(jnp.float32)
    normed = (widened * lax.rsqrt(lax.optimization_barrier(jnp.mean(widened * widened, axis=1, keepdims=True)) + 1e-06)).astype(jnp.bfloat16)
    pre_units = jnp.dot(normed, up_round, preferred_element_type=jnp.float32)
    act_units = jnp.square(jax.nn.relu(pre_units)).astype(jnp.bfloat16)
    mixed = lax.dot_general(act_units, down_round, (((1,), (1,)), ((), ())), preferred_element_type=jnp.float32)
    return (sampled(up_round), sampled(down_round), mixed.astype(jnp.bfloat16))
```

```python
import jax
import jax.numpy as jnp
import numpy as np
from jax import lax
from jax.sharding import Mesh
from jax.sharding import PartitionSpec as P

SUB = 8
ROOM = 2.0**15
COARSE = 14
SPARE = 8


def power_scale(largest):
    scale = jnp.ones_like(largest)
    factors = []
    for _ in range(SPARE - 1):
        fits = largest * (scale * 2.0**COARSE) < ROOM
        scale = jnp.where(fits, scale * 2.0**COARSE, scale)
        factors.append(jnp.where(fits, 2.0**-COARSE, 1.0))
    last = jnp.ones_like(largest)
    for step in (8, 4, 2):
        fits = largest * (scale * 2.0**step) < ROOM
        scale = jnp.where(fits, scale * 2.0**step, scale)
        last = jnp.where(fits, last * 2.0**-step, last)
    factors.append(last)
    return scale, jnp.stack(factors)


def on_device(tokens, gain, up_master, down_master):
    feat_rows = up_master.shape[0]
    units = up_master.shape[1] // SUB
    x_count = lax.axis_size("x")
    y_count = lax.axis_size("y")
    rows, width = tokens.shape
    up_round = (gain[:, None] * up_master).astype(jnp.bfloat16)
    down_round = down_master.astype(jnp.bfloat16)
    both = jnp.concatenate(
        [up_round.reshape(feat_rows, SUB, units), down_round.reshape(feat_rows, SUB, units)], axis=2
    ).transpose(1, 0, 2)
    both = lax.all_to_all(both, ("x", "c"), 0, 0, tiled=True)
    block = both.reshape(SUB * feat_rows, 2 * units).astype(jnp.float32)

    widened = tokens.astype(jnp.float32)
    normed = (
        widened * lax.rsqrt(jnp.mean(widened * widened, axis=1, keepdims=True) + 1e-06)
    ).astype(jnp.bfloat16)
    held = [normed]
    for ahead in range(1, x_count):
        held.append(lax.ppermute(normed, "x", [((i + ahead) % x_count, i) for i in range(x_count)]))

    scale, factors = power_scale(jnp.max(jnp.abs(block), axis=0))
    packed = jnp.concatenate([block * scale, factors]).astype(jnp.float16)
    spread = lax.all_gather(packed[None], ("z", "c"), axis=0, tiled=True)
    spread = spread.reshape(-1, 2, SUB * feat_rows + SPARE, 2 * units).astype(jnp.float32)
    inverse = jnp.prod(spread[:, :, SUB * feat_rows :], axis=2, keepdims=True)
    weights = (spread[:, :, : SUB * feat_rows] * inverse).astype(jnp.bfloat16)
    core = lax.axis_index("c")
    mine, other = (
        lax.dynamic_index_in_dim(weights, which, 1, keepdims=False).reshape(width, 2 * units)
        for which in (core, 1 - core)
    )
    gathered = jnp.concatenate(held)
    partial_out = 0.0
    for pair in (mine, other):
        pre_units = jnp.dot(gathered, pair[:, :units], preferred_element_type=jnp.float32)
        act_units = jnp.square(jax.nn.relu(pre_units)).astype(jnp.bfloat16)
        partial_out += lax.dot_general(
            act_units, pair[:, units:], (((1,), (1,)), ((), ())), preferred_element_type=jnp.float32
        )
    pieces = partial_out.astype(jnp.bfloat16).reshape(x_count, rows, y_count, width // y_count)
    pieces = jnp.roll(pieces.transpose(0, 2, 1, 3), lax.axis_index("x"), axis=0)
    pieces = pieces.reshape(x_count * y_count, rows, width // y_count)
    pieces = lax.all_to_all(pieces, ("x", "y"), 0, 0, tiled=True)
    mixed = jnp.sum(pieces.astype(jnp.float32), axis=0).astype(jnp.bfloat16)
    return mine[None, :, :units], mine[None, :, units:], mixed


def solution(mesh):
    fine = Mesh(np.reshape(mesh.devices, (16, 4, 2, 4)), ("z", "x", "c", "y"))
    fs = ("z", "x", "c")
    return jax.shard_map(
        on_device,
        mesh=fine,
        in_specs=(P(fs, None), P(fs), P(fs, "y"), P(fs, "y")),
        out_specs=(P(fs, None, "y"), P(fs, None, "y"), P(fs, "y")),
        check_vma=False,
    )
```

```python
import functools

import jax
import jax.numpy as jnp
import numpy as np
from jax import lax
from jax.experimental import pallas as pl
from jax.experimental.pallas import tpu as pltpu
from jax.sharding import Mesh
from jax.sharding import PartitionSpec as P

SUB = 8
ROOM = 2.0**15
COARSE = 14
SPARE = 8


def power_scale(largest):
    scale = jnp.ones_like(largest)
    factors = []
    for _ in range(SPARE - 1):
        fits = largest * (scale * 2.0**COARSE) < ROOM
        scale = jnp.where(fits, scale * 2.0**COARSE, scale)
        factors.append(jnp.where(fits, 2.0**-COARSE, 1.0))
    last = jnp.ones_like(largest)
    for step in (8, 4, 2):
        fits = largest * (scale * 2.0**step) < ROOM
        scale = jnp.where(fits, scale * 2.0**step, scale)
        last = jnp.where(fits, last * 2.0**-step, last)
    factors.append(last)
    return scale, jnp.stack(factors)


def apply_kernel(units, core_ref, tokens, spread, up_out, down_out, pieces, up, down, hidden, sems):
    core = core_ref[0]
    x_count, rows, width = tokens.shape
    y_count = pieces.shape[0] // x_count
    feats = spread.shape[1] - SPARE
    part = width // y_count

    def unpack(z, carry):
        for half in range(2):
            packed = spread[2 * z + (core if half == 0 else 1 - core)].astype(jnp.float32)
            inverse = packed[feats : feats + 1]
            for k in range(1, SPARE):
                inverse = inverse * packed[feats + k : feats + k + 1]
            values = (packed[:feats] * inverse).astype(jnp.bfloat16)
            at = pl.ds(pl.multiple_of(z * feats, feats), feats)
            up[at, half * units : (half + 1) * units] = values[:, :units]
            down[at, half * units : (half + 1) * units] = values[:, units:]
        return carry

    lax.fori_loop(0, width // feats, unpack, 0)
    hidden[...] = jnp.zeros_like(hidden)

    for k in range(y_count):
        cols = slice(k * part, (k + 1) * part)
        hidden[...] += jnp.dot(
            tokens[:, :, cols].reshape(x_count * rows, part),
            up[cols, :],
            preferred_element_type=jnp.float32,
        )
    copies = [
        pltpu.make_async_copy(source.at[:, :units], target, sems.at[i])
        for i, (source, target) in enumerate(((up, up_out), (down, down_out)))
    ]
    for copy in copies:
        copy.start()
    act = jnp.square(jnp.maximum(hidden[...], 0.0)).astype(jnp.bfloat16)
    for y in range(y_count):
        out = lax.dot_general(
            act,
            down[y * part : (y + 1) * part, :],
            (((1,), (1,)), ((), ())),
            preferred_element_type=jnp.float32,
        ).astype(jnp.bfloat16)
        for x in range(x_count):
            pieces[x * y_count + y] = out[x * rows : (x + 1) * rows]
    for copy in copies:
        copy.wait()


def apply(core, tokens, spread, y_count):
    x_count, rows, width = tokens.shape
    units = spread.shape[2] // 2
    weight = jax.ShapeDtypeStruct((width, units), jnp.bfloat16)
    vmem = pl.BlockSpec(memory_space=pltpu.VMEM)
    anywhere = pl.BlockSpec(memory_space=pl.ANY)
    return pl.pallas_call(
        functools.partial(apply_kernel, units),
        out_shape=(
            weight,
            weight,
            jax.ShapeDtypeStruct((x_count * y_count, rows, width // y_count), jnp.bfloat16),
        ),
        in_specs=[pl.BlockSpec(memory_space=pltpu.SMEM), vmem, vmem],
        out_specs=(anywhere, anywhere, vmem),
        scratch_shapes=[
            pltpu.VMEM((width, 2 * units), jnp.bfloat16),
            pltpu.VMEM((width, 2 * units), jnp.bfloat16),
            pltpu.VMEM((x_count * rows, 2 * units), jnp.float32),
            pltpu.SemaphoreType.DMA((2,)),
        ],
        cost_estimate=pl.CostEstimate(
            flops=8 * x_count * rows * width * units, bytes_accessed=16 << 20, transcendentals=0
        ),
        compiler_params=pltpu.CompilerParams(vmem_limit_bytes=40 << 20),
    )(core, tokens, spread)


def on_device(tokens, gain, up_master, down_master):
    feat_rows = up_master.shape[0]
    units = up_master.shape[1] // SUB
    x_count = lax.axis_size("x")
    y_count = lax.axis_size("y")
    up_round = (gain[:, None] * up_master).astype(jnp.bfloat16)
    down_round = down_master.astype(jnp.bfloat16)
    both = jnp.concatenate(
        [up_round.reshape(feat_rows, SUB, units), down_round.reshape(feat_rows, SUB, units)], axis=2
    ).transpose(1, 0, 2)
    both = lax.all_to_all(both, ("x", "c"), 0, 0, tiled=True)

    widened = tokens.astype(jnp.float32)
    normed = (
        widened * lax.rsqrt(jnp.mean(widened * widened, axis=1, keepdims=True) + 1e-06)
    ).astype(jnp.bfloat16)
    copies = jnp.broadcast_to(normed[None], (x_count, *normed.shape))
    both, copies = lax.optimization_barrier((both, copies))
    gathered = lax.all_to_all(copies, "x", 0, 0, tiled=True)

    block = both.reshape(SUB * feat_rows, 2 * units).astype(jnp.float32)
    scale, factors = power_scale(jnp.max(jnp.abs(block), axis=0))
    packed = jnp.concatenate([block * scale, factors]).astype(jnp.float16)
    spread = lax.all_gather(packed[None], ("z", "c"), axis=0, tiled=True)
    core = lax.axis_index("c").astype(jnp.int32)[None]
    up_own, down_own, pieces = apply(core, gathered, spread.astype(jnp.bfloat16), y_count)
    pieces = lax.all_to_all(pieces, ("x", "y"), 0, 0, tiled=True)
    mixed = jnp.sum(pieces.astype(jnp.float32), axis=0).astype(jnp.bfloat16)
    return up_own[None], down_own[None], mixed


def solution(mesh):
    fine = Mesh(np.reshape(mesh.devices, (16, 4, 2, 4)), ("z", "x", "c", "y"))
    fs = ("z", "x", "c")
    return jax.shard_map(
        on_device,
        mesh=fine,
        in_specs=(P(fs, None), P(fs), P(fs, "y"), P(fs, "y")),
        out_specs=(P(fs, None, "y"), P(fs, None, "y"), P(fs, "y")),
        check_vma=False,
    )
```

```python
import functools

import jax
import jax.numpy as jnp
import numpy as np
from jax import lax
from jax.experimental import pallas as pl
from jax.experimental.pallas import tpu as pltpu
from jax.sharding import Mesh
from jax.sharding import PartitionSpec as P

SUB = 8
ROOM = 2.0**15
COARSE = 14
SPARE = 8


def power_scale(largest):
    scale = jnp.ones_like(largest)
    factors = []
    for _ in range(SPARE - 1):
        fits = largest * (scale * 2.0**COARSE) < ROOM
        scale = jnp.where(fits, scale * 2.0**COARSE, scale)
        factors.append(jnp.where(fits, 2.0**-COARSE, 1.0))
    last = jnp.ones_like(largest)
    for step in (8, 4, 2):
        fits = largest * (scale * 2.0**step) < ROOM
        scale = jnp.where(fits, scale * 2.0**step, scale)
        last = jnp.where(fits, last * 2.0**-step, last)
    factors.append(last)
    return scale, jnp.stack(factors)


def fold_kernel(gain, up, down, out):
    members, _, columns = out.shape
    units = columns // 2
    for m in range(members):
        at = slice(m * units, (m + 1) * units)
        out[m, :, :units] = (gain[...] * up[:, at]).astype(jnp.bfloat16)
        out[m, :, units:] = down[:, at].astype(jnp.bfloat16)


def fold(gain, up, down):
    rows, columns = up.shape
    return pl.pallas_call(
        fold_kernel,
        out_shape=jax.ShapeDtypeStruct((SUB, rows, 2 * columns // SUB), jnp.bfloat16),
        cost_estimate=pl.CostEstimate(
            flops=2 * up.size, bytes_accessed=12 * up.size, transcendentals=0
        ),
        compiler_params=pltpu.CompilerParams(vmem_limit_bytes=4 << 20),
    )(gain, up, down)


def norm_kernel(tokens, out, normed, sems):
    widened = tokens[...].astype(jnp.float32)
    mean = jnp.mean(widened * widened, axis=1, keepdims=True)
    normed[...] = (widened * lax.rsqrt(mean + 1e-06)).astype(jnp.bfloat16)
    copies = [pltpu.make_async_copy(normed, out.at[x], sems.at[x]) for x in range(out.shape[0])]
    for copy in copies:
        copy.start()
    for copy in copies:
        copy.wait()


def norm_copies(tokens, count):
    return pl.pallas_call(
        norm_kernel,
        out_shape=jax.ShapeDtypeStruct((count, *tokens.shape), jnp.bfloat16),
        out_specs=pl.BlockSpec(memory_space=pltpu.HBM),
        scratch_shapes=[
            pltpu.VMEM(tokens.shape, jnp.bfloat16),
            pltpu.SemaphoreType.DMA((count,)),
        ],
        cost_estimate=pl.CostEstimate(
            flops=2_000_000_000, bytes_accessed=10 * tokens.size, transcendentals=tokens.shape[0]
        ),
        compiler_params=pltpu.CompilerParams(vmem_limit_bytes=8 << 20),
    )(tokens)


def apply_kernel(units, core_ref, tokens, weights, up_out, down_out, pieces, up, down, hidden, sems):
    core = core_ref[0]
    x_count, rows, width = tokens.shape
    y_count = pieces.shape[0] // x_count
    feats = weights.shape[1]
    part = width // y_count

    def unpack(z, carry):
        for half in range(2):
            values = weights[2 * z + (core if half == 0 else 1 - core)]
            at = pl.ds(pl.multiple_of(z * feats, feats), feats)
            up[at, half * units : (half + 1) * units] = values[:, :units]
            down[at, half * units : (half + 1) * units] = values[:, units:]
        return carry

    lax.fori_loop(0, width // feats, unpack, 0)
    hidden[...] = jnp.zeros_like(hidden)

    for k in range(y_count):
        cols = slice(k * part, (k + 1) * part)
        hidden[...] += jnp.dot(
            tokens[:, :, cols].reshape(x_count * rows, part),
            up[cols, :],
            preferred_element_type=jnp.float32,
        )
    copies = [
        pltpu.make_async_copy(source.at[:, :units], target, sems.at[i])
        for i, (source, target) in enumerate(((up, up_out), (down, down_out)))
    ]
    for copy in copies:
        copy.start()
    act = jnp.square(jnp.maximum(hidden[...], 0.0)).astype(jnp.bfloat16)
    for y in range(y_count):
        out = lax.dot_general(
            act,
            down[y * part : (y + 1) * part, :],
            (((1,), (1,)), ((), ())),
            preferred_element_type=jnp.float32,
        ).astype(jnp.bfloat16)
        for x in range(x_count):
            pieces[x * y_count + y] = out[x * rows : (x + 1) * rows]
    for copy in copies:
        copy.wait()


def apply(core, tokens, weights, y_count):
    x_count, rows, width = tokens.shape
    units = weights.shape[2] // 2
    weight = jax.ShapeDtypeStruct((width, units), jnp.bfloat16)
    vmem = pl.BlockSpec(memory_space=pltpu.VMEM)
    anywhere = pl.BlockSpec(memory_space=pl.ANY)
    return pl.pallas_call(
        functools.partial(apply_kernel, units),
        out_shape=(
            weight,
            weight,
            jax.ShapeDtypeStruct((x_count * y_count, rows, width // y_count), jnp.bfloat16),
        ),
        in_specs=[pl.BlockSpec(memory_space=pltpu.SMEM), vmem, vmem],
        out_specs=(anywhere, anywhere, vmem),
        scratch_shapes=[
            pltpu.VMEM((width, 2 * units), jnp.bfloat16),
            pltpu.VMEM((width, 2 * units), jnp.bfloat16),
            pltpu.VMEM((x_count * rows, 2 * units), jnp.float32),
            pltpu.SemaphoreType.DMA((2,)),
        ],
        cost_estimate=pl.CostEstimate(
            flops=8 * x_count * rows * width * units, bytes_accessed=16 << 20, transcendentals=0
        ),
        compiler_params=pltpu.CompilerParams(vmem_limit_bytes=20 << 20),
    )(core, tokens, weights)


def on_device(tokens, gain, up_master, down_master):
    feat_rows = up_master.shape[0]
    units = up_master.shape[1] // SUB
    feats = SUB * feat_rows
    x_count = lax.axis_size("x")
    y_count = lax.axis_size("y")
    both = fold(gain[:, None], up_master, down_master)
    both = lax.all_to_all(both, ("x", "c"), 0, 0, tiled=True)
    gathered = lax.all_to_all(norm_copies(tokens, x_count), "x", 0, 0, tiled=True)

    block = both.reshape(feats, 2 * units).astype(jnp.float32)
    scale, factors = power_scale(jnp.max(jnp.abs(block), axis=0))
    packed = jnp.concatenate([block * scale, factors]).astype(jnp.float16)
    spread = lax.all_gather(packed[None], ("z", "c"), axis=0, tiled=True)
    spread, gathered = lax.optimization_barrier((spread, gathered))
    tail = lax.optimization_barrier(spread[:, feats:])
    inverse = jnp.prod(tail.astype(jnp.float32), axis=1, keepdims=True)
    weights = (spread[:, :feats].astype(jnp.float32) * inverse).astype(jnp.bfloat16)
    core = lax.axis_index("c").astype(jnp.int32)[None]
    up_own, down_own, pieces = apply(core, gathered, weights, y_count)
    pieces = lax.all_to_all(pieces, ("x", "y"), 0, 0, tiled=True)
    mixed = jnp.sum(pieces.astype(jnp.float32), axis=0).astype(jnp.bfloat16)
    return up_own[None], down_own[None], mixed


def solution(mesh):
    fine = Mesh(np.reshape(mesh.devices, (16, 4, 2, 4)), ("z", "x", "c", "y"))
    fs = ("z", "x", "c")
    return jax.shard_map(
        on_device,
        mesh=fine,
        in_specs=(P(fs, None), P(fs), P(fs, "y"), P(fs, "y")),
        out_specs=(P(fs, None, "y"), P(fs, None, "y"), P(fs, "y")),
        check_vma=False,
    )
```

```python
import functools

import jax
import jax.numpy as jnp
import numpy as np
from jax import lax
from jax.experimental import pallas as pl
from jax.experimental.pallas import tpu as pltpu
from jax.sharding import Mesh
from jax.sharding import PartitionSpec as P

SUB = 8
ROOM = 2.0**15
COARSE = 14
SPARE = 8


def power_scale(largest):
    scale = jnp.ones_like(largest)
    factors = []
    for _ in range(SPARE - 1):
        fits = largest * (scale * 2.0**COARSE) < ROOM
        scale = jnp.where(fits, scale * 2.0**COARSE, scale)
        factors.append(jnp.where(fits, 2.0**-COARSE, 1.0))
    last = jnp.ones_like(largest)
    for step in (8, 4, 2):
        fits = largest * (scale * 2.0**step) < ROOM
        scale = jnp.where(fits, scale * 2.0**step, scale)
        last = jnp.where(fits, last * 2.0**-step, last)
    factors.append(last)
    return scale, jnp.stack(factors)


def fold_kernel(gain_in, up_in, down_in, out, gain, up, down, sems):
    loads = [
        pltpu.make_async_copy(source, target, sems.at[i])
        for i, (source, target) in enumerate(
            ((gain_in, gain), (up_in, up), (down_in, down))
        )
    ]
    for load in loads:
        load.start()
    for load in loads:
        load.wait()
    members, rows, columns = out.shape
    units = columns // 2
    square = (rows, rows)
    here = lax.broadcasted_iota(jnp.int32, square, 0) == lax.broadcasted_iota(jnp.int32, square, 1)
    spread = jnp.sum(jnp.where(here, jnp.broadcast_to(gain[...], square), 0.0), axis=1, keepdims=True)
    for m in range(members):
        at = slice(m * units, (m + 1) * units)
        out[m, :, :units] = (spread * up[:, at]).astype(jnp.bfloat16)
        out[m, :, units:] = down[:, at].astype(jnp.bfloat16)


def fold(gain, up, down):
    rows, columns = up.shape
    return pl.pallas_call(
        fold_kernel,
        out_shape=jax.ShapeDtypeStruct((SUB, rows, 2 * columns // SUB), jnp.bfloat16),
        in_specs=[pl.BlockSpec(memory_space=pl.ANY)] * 3,
        scratch_shapes=[
            pltpu.VMEM(gain.shape, jnp.float32),
            pltpu.VMEM(up.shape, jnp.float32),
            pltpu.VMEM(up.shape, jnp.float32),
            pltpu.SemaphoreType.DMA((3,)),
        ],
        cost_estimate=pl.CostEstimate(
            flops=2 * up.size, bytes_accessed=12 * up.size, transcendentals=0
        ),
    )(gain, up, down)


def norm_kernel(tokens, out, normed, sems):
    widened = tokens[...].astype(jnp.float32)
    mean = jnp.mean(widened * widened, axis=1, keepdims=True)
    normed[...] = (widened * lax.rsqrt(mean + 1e-06)).astype(jnp.bfloat16)
    copies = [pltpu.make_async_copy(normed, out.at[x], sems.at[x]) for x in range(out.shape[0])]
    for copy in copies:
        copy.start()
    for copy in copies:
        copy.wait()


def norm_copies(tokens, count):
    return pl.pallas_call(
        norm_kernel,
        out_shape=jax.ShapeDtypeStruct((count, *tokens.shape), jnp.bfloat16),
        out_specs=pl.BlockSpec(memory_space=pltpu.HBM),
        scratch_shapes=[
            pltpu.VMEM(tokens.shape, jnp.bfloat16),
            pltpu.SemaphoreType.DMA((count,)),
        ],
        cost_estimate=pl.CostEstimate(
            flops=2_000_000_000, bytes_accessed=10 * tokens.size, transcendentals=tokens.shape[0]
        ),
    )(tokens)


def apply_kernel(units, core_ref, tokens, weights, up_out, down_out, pieces, up, down, hidden, sems):
    core = core_ref[0]
    x_count, rows, width = tokens.shape
    y_count = pieces.shape[0] // x_count
    feats = weights.shape[1] - SPARE
    part = width // y_count

    def unpack(z, carry):
        for half in range(2):
            packed = weights[2 * z + (core if half == 0 else 1 - core)]
            inverse = packed[feats : feats + 1]
            for k in range(1, SPARE):
                inverse = inverse * packed[feats + k : feats + k + 1]
            values = (packed[:feats] * inverse).astype(jnp.bfloat16)
            at = pl.ds(pl.multiple_of(z * feats, feats), feats)
            up[at, half * units : (half + 1) * units] = values[:, :units]
            down[at, half * units : (half + 1) * units] = values[:, units:]
        return carry

    lax.fori_loop(0, width // feats, unpack, 0)
    hidden[...] = jnp.zeros_like(hidden)

    for k in range(y_count):
        cols = slice(k * part, (k + 1) * part)
        hidden[...] += jnp.dot(
            tokens[:, :, cols].reshape(x_count * rows, part),
            up[cols, :],
            preferred_element_type=jnp.float32,
        )
    copies = [
        pltpu.make_async_copy(source.at[:, :units], target, sems.at[i])
        for i, (source, target) in enumerate(((up, up_out), (down, down_out)))
    ]
    for copy in copies:
        copy.start()
    act = jnp.square(jnp.maximum(hidden[...], 0.0)).astype(jnp.bfloat16)
    for y in range(y_count):
        out = lax.dot_general(
            act,
            down[y * part : (y + 1) * part, :],
            (((1,), (1,)), ((), ())),
            preferred_element_type=jnp.float32,
        ).astype(jnp.bfloat16)
        for x in range(x_count):
            place = jnp.where(core == 0, x * y_count + y, y * x_count + x)
            pieces[place] = out[x * rows : (x + 1) * rows]
    for copy in copies:
        copy.wait()


def apply(core, tokens, weights, y_count):
    x_count, rows, width = tokens.shape
    units = weights.shape[2] // 2
    weight = jax.ShapeDtypeStruct((width, units), jnp.bfloat16)
    vmem = pl.BlockSpec(memory_space=pltpu.VMEM)
    anywhere = pl.BlockSpec(memory_space=pl.ANY)
    return pl.pallas_call(
        functools.partial(apply_kernel, units),
        out_shape=(
            weight,
            weight,
            jax.ShapeDtypeStruct((x_count * y_count, rows, width // y_count), jnp.bfloat16),
        ),
        in_specs=[pl.BlockSpec(memory_space=pltpu.SMEM), vmem, vmem],
        out_specs=(anywhere, anywhere, vmem),
        scratch_shapes=[
            pltpu.VMEM((width, 2 * units), jnp.bfloat16),
            pltpu.VMEM((width, 2 * units), jnp.bfloat16),
            pltpu.VMEM((x_count * rows, 2 * units), jnp.float32),
            pltpu.SemaphoreType.DMA((2,)),
        ],
        cost_estimate=pl.CostEstimate(
            flops=8 * x_count * rows * width * units, bytes_accessed=16 << 20, transcendentals=0
        ),
        compiler_params=pltpu.CompilerParams(vmem_limit_bytes=24 << 20),
    )(core, tokens, weights)


def crossed_groups(x_count, y_count):
    def at(x, c, y):
        return (x * 2 + c) * y_count + y

    def along_x(c):
        return [[at(x, c, y) for x in range(x_count)] for y in range(y_count)]

    def along_y(c):
        return [[at(x, c, y) for y in range(y_count)] for x in range(x_count)]

    return along_x(0) + along_y(1), along_y(0) + along_x(1)


def on_device(tokens, gain, up_master, down_master):
    feat_rows = up_master.shape[0]
    units = up_master.shape[1] // SUB
    feats = SUB * feat_rows
    x_count = lax.axis_size("x")
    y_count = lax.axis_size("y")
    both = fold(gain[None], up_master, down_master)
    both = lax.all_to_all(both, ("x", "c"), 0, 0, tiled=True)
    gathered = lax.all_to_all(norm_copies(tokens, x_count), "x", 0, 0, tiled=True)

    block = both.reshape(feats, 2 * units).astype(jnp.float32)
    scale, factors = power_scale(jnp.max(jnp.abs(block), axis=0))
    packed = jnp.concatenate([block * scale, factors]).astype(jnp.float16)
    spread = lax.all_gather(packed[None], ("z", "c"), axis=0, tiled=True)
    spread, gathered = lax.optimization_barrier((spread, gathered))
    core = lax.axis_index("c").astype(jnp.int32)[None]
    up_own, down_own, pieces = apply(core, gathered, spread.astype(jnp.float32), y_count)
    for groups in crossed_groups(x_count, y_count):
        pieces = lax.all_to_all(
            pieces, ("x", "c", "y"), 0, 0, tiled=True, axis_index_groups=groups
        )
        pieces = pieces.reshape(len(groups[0]), -1, *pieces.shape[1:])
        pieces = jnp.sum(pieces.astype(jnp.float32), axis=0).astype(jnp.bfloat16)
    return up_own[None], down_own[None], pieces[0]


def solution(mesh):
    fine = Mesh(np.reshape(mesh.devices, (16, 4, 2, 4)), ("z", "x", "c", "y"))
    fs = ("z", "x", "c")
    return jax.shard_map(
        on_device,
        mesh=fine,
        in_specs=(P(fs, None), P(fs), P(fs, "y"), P(fs, "y")),
        out_specs=(P(fs, None, "y"), P(fs, None, "y"), P(fs, "y")),
        check_vma=False,
    )
```

```python
import functools

import jax
import jax.numpy as jnp
import numpy as np
from jax import lax
from jax.experimental import pallas as pl
from jax.experimental.pallas import tpu as pltpu
from jax.sharding import Mesh
from jax.sharding import PartitionSpec as P

SUB = 8
LANES = 128
ROOM = 2.0**15
FACTORS = 4
REACH = 28
GRANT = 47 << 20


def power_scale(largest):
    scale = jnp.ones_like(largest)
    factors = []
    for _ in range(FACTORS - 1):
        fits = largest * (scale * 2.0**REACH) < ROOM
        scale = jnp.where(fits, scale * 2.0**REACH, scale)
        factors.append(jnp.where(fits, ROOM * 2.0**-REACH, ROOM))
    last = jnp.full_like(largest, ROOM)
    for step in (16, 8, 4):
        fits = largest * (scale * 2.0**step) < ROOM
        scale = jnp.where(fits, scale * 2.0**step, scale)
        last = jnp.where(fits, last * 2.0**-step, last)
    factors.append(last)
    return scale, jnp.stack(factors, axis=1)


def fold_kernel(gain_in, up_in, down_in, out, gain, up, down, sems):
    loads = [
        pltpu.make_async_copy(source, target, sems.at[i])
        for i, (source, target) in enumerate(((gain_in, gain), (up_in, up), (down_in, down)))
    ]
    for load in loads:
        load.start()
    for load in loads:
        load.wait()
    chips, double, rows, _ = out.shape
    slabs = double // 2
    square = (rows, rows)
    here = lax.broadcasted_iota(jnp.int32, square, 0) == lax.broadcasted_iota(jnp.int32, square, 1)
    spread = jnp.sum(jnp.where(here, jnp.broadcast_to(gain[...], square), 0.0), axis=1, keepdims=True)
    for x in range(chips):
        for slab in range(slabs):
            first = (x * slabs + slab) * LANES
            out[x, slab] = (spread * up[:, first : first + LANES]).astype(jnp.bfloat16)
            out[x, slabs + slab] = down[:, first : first + LANES].astype(jnp.bfloat16)


def fold(gain, up, down, chips):
    rows, columns = up.shape
    slabs = columns // chips // LANES
    return pl.pallas_call(
        fold_kernel,
        out_shape=jax.ShapeDtypeStruct((chips, 2 * slabs, rows, LANES), jnp.bfloat16),
        in_specs=[pl.BlockSpec(memory_space=pl.ANY)] * 3,
        scratch_shapes=[
            pltpu.VMEM(gain.shape, jnp.float32),
            pltpu.VMEM(up.shape, jnp.float32),
            pltpu.VMEM(up.shape, jnp.float32),
            pltpu.SemaphoreType.DMA((3,)),
        ],
        cost_estimate=pl.CostEstimate(
            flops=2 * up.size, bytes_accessed=12 * up.size, transcendentals=0
        ),
    )(gain, up, down)


def norm_kernel(tokens, out, normed, sems):
    widened = tokens[...].astype(jnp.float32)
    mean = jnp.mean(widened * widened, axis=1, keepdims=True)
    normed[...] = (widened * lax.rsqrt(mean + 1e-06)).astype(jnp.bfloat16)
    copies = [pltpu.make_async_copy(normed, out.at[x], sems.at[x]) for x in range(out.shape[0])]
    for copy in copies:
        copy.start()
    for copy in copies:
        copy.wait()


def norm_copies(tokens, count):
    return pl.pallas_call(
        norm_kernel,
        out_shape=jax.ShapeDtypeStruct((count, *tokens.shape), jnp.bfloat16),
        out_specs=pl.BlockSpec(memory_space=pltpu.HBM),
        scratch_shapes=[
            pltpu.VMEM(tokens.shape, jnp.bfloat16),
            pltpu.SemaphoreType.DMA((count,)),
        ],
        cost_estimate=pl.CostEstimate(
            flops=2_000_000_000, bytes_accessed=10 * tokens.size, transcendentals=tokens.shape[0]
        ),
    )(tokens)


def apply_kernel(
    feat_rows, core_ref, tokens, weights, up_out, down_out, pieces, held, up, down, hidden, load_sems, sems
):
    core = core_ref[0]
    x_count, rows, width = tokens.shape
    y_count = pieces.shape[0] // x_count
    part = width // y_count
    units = up_out.shape[1]
    z_count = held.shape[0]
    slab_rows = x_count * feat_rows
    unit_slabs = units // LANES
    slabs = 2 * unit_slabs
    last = 2 * slabs * slab_rows

    def load(z):
        return pltpu.make_async_copy(weights.at[z], held.at[z], load_sems.at[z])

    for z in range(z_count):
        load(z).start()

    def unpack(z, carry):
        load(z).wait()
        for source in range(2):
            for matrix, target in enumerate((up, down)):
                first = last + matrix * FACTORS
                factors = held[z, source, first : first + FACTORS].astype(jnp.float32)
                inverse = factors[0:1] * ROOM**-FACTORS
                for k in range(1, FACTORS):
                    inverse = inverse * factors[k : k + 1]
                for half in range(2):
                    member = core if half == 0 else 1 - core
                    for j in range(unit_slabs):
                        slab = matrix * slabs + member * unit_slabs + j
                        start = pl.multiple_of(slab * slab_rows, slab_rows)
                        packed = held[z, source, pl.ds(start, slab_rows)].astype(jnp.float32)
                        values = (packed * inverse).astype(jnp.bfloat16)
                        column = half * units + j * LANES
                        for x in range(x_count):
                            row = ((z * x_count + x) * 2 + source) * feat_rows
                            target[pl.ds(pl.multiple_of(row, feat_rows), feat_rows), column : column + LANES] = (
                                values[x * feat_rows : (x + 1) * feat_rows]
                            )
        return carry

    lax.fori_loop(0, z_count, unpack, 0)
    hidden[...] = jnp.zeros_like(hidden)
    for k in range(y_count):
        cols = slice(k * part, (k + 1) * part)
        hidden[...] += jnp.dot(
            tokens[:, :, cols].reshape(x_count * rows, part),
            up[cols, :],
            preferred_element_type=jnp.float32,
        )
    copies = [
        pltpu.make_async_copy(source.at[:, :units], target, sems.at[i])
        for i, (source, target) in enumerate(((up, up_out), (down, down_out)))
    ]
    for copy in copies:
        copy.start()
    act = jnp.square(jnp.maximum(hidden[...], 0.0)).astype(jnp.bfloat16)
    for y in range(y_count):
        out = lax.dot_general(
            act,
            down[y * part : (y + 1) * part, :],
            (((1,), (1,)), ((), ())),
            preferred_element_type=jnp.float32,
        ).astype(jnp.bfloat16)
        for x in range(x_count):
            place = jnp.where(core == 0, x * y_count + y, y * x_count + x)
            pieces[place] = out[x * rows : (x + 1) * rows]
    for copy in copies:
        copy.wait()


def apply(core, tokens, weights, units, feat_rows, y_count):
    x_count, rows, width = tokens.shape
    weight = jax.ShapeDtypeStruct((width, units), jnp.bfloat16)
    vmem = pl.BlockSpec(memory_space=pltpu.VMEM)
    anywhere = pl.BlockSpec(memory_space=pl.ANY)
    return pl.pallas_call(
        functools.partial(apply_kernel, feat_rows),
        out_shape=(
            weight,
            weight,
            jax.ShapeDtypeStruct((x_count * y_count, rows, width // y_count), jnp.bfloat16),
        ),
        in_specs=[pl.BlockSpec(memory_space=pltpu.SMEM), vmem, anywhere],
        out_specs=(anywhere, anywhere, vmem),
        scratch_shapes=[
            pltpu.VMEM(weights.shape, jnp.bfloat16),
            pltpu.VMEM((width, 2 * units), jnp.bfloat16),
            pltpu.VMEM((width, 2 * units), jnp.bfloat16),
            pltpu.VMEM((x_count * rows, 2 * units), jnp.float32),
            pltpu.SemaphoreType.DMA((weights.shape[0],)),
            pltpu.SemaphoreType.DMA((2,)),
        ],
        cost_estimate=pl.CostEstimate(
            flops=8 * x_count * rows * width * units, bytes_accessed=16 << 20, transcendentals=0
        ),
        compiler_params=pltpu.CompilerParams(vmem_limit_bytes=GRANT),
    )(core, tokens, weights)


def crossed_groups(x_count, y_count):
    def at(x, c, y):
        return (x * 2 + c) * y_count + y

    def along_x(c):
        return [[at(x, c, y) for x in range(x_count)] for y in range(y_count)]

    def along_y(c):
        return [[at(x, c, y) for y in range(y_count)] for x in range(x_count)]

    return along_x(0) + along_y(1), along_y(0) + along_x(1)


def on_device(tokens, gain, up_master, down_master):
    feat_rows = up_master.shape[0]
    units = up_master.shape[1] // SUB
    x_count = lax.axis_size("x")
    y_count = lax.axis_size("y")
    both = fold(gain[None], up_master, down_master, x_count)
    both = lax.all_to_all(both, "x", 0, 0, tiled=True)
    gathered = lax.all_to_all(norm_copies(tokens, x_count), "x", 0, 0, tiled=True)

    block = both.astype(jnp.float32).reshape(x_count, 2, -1, feat_rows, LANES)
    scale, factors = power_scale(jnp.max(jnp.abs(block), axis=(0, 2, 3)))
    packed = (block * scale[None, :, None, None]).transpose(1, 2, 0, 3, 4).reshape(-1, LANES)
    packed = jnp.concatenate([packed, factors.reshape(-1, LANES)]).astype(jnp.float16)
    spread = lax.all_gather(packed[None], ("z", "c"), axis=0, tiled=True)
    spread = spread.reshape(-1, 2, *packed.shape).astype(jnp.bfloat16)
    core = lax.axis_index("c").astype(jnp.int32)[None]
    up_own, down_own, pieces = apply(core, gathered, spread, units, feat_rows, y_count)
    for groups in crossed_groups(x_count, y_count):
        pieces = lax.all_to_all(
            pieces, ("x", "c", "y"), 0, 0, tiled=True, axis_index_groups=groups
        )
        pieces = pieces.reshape(len(groups[0]), -1, *pieces.shape[1:])
        pieces = jnp.sum(pieces.astype(jnp.float32), axis=0).astype(jnp.bfloat16)
    return up_own[None], down_own[None], pieces[0]


def solution(mesh):
    fine = Mesh(np.reshape(mesh.devices, (16, 4, 2, 4)), ("z", "x", "c", "y"))
    fs = ("z", "x", "c")
    return jax.shard_map(
        on_device,
        mesh=fine,
        in_specs=(P(fs, None), P(fs), P(fs, "y"), P(fs, "y")),
        out_specs=(P(fs, None, "y"), P(fs, None, "y"), P(fs, "y")),
        check_vma=False,
    )
```

```python
import functools

import jax
import jax.numpy as jnp
import numpy as np
from jax import lax
from jax.experimental import pallas as pl
from jax.experimental.pallas import tpu as pltpu
from jax.sharding import Mesh
from jax.sharding import PartitionSpec as P

SUB = 8
LANES = 128
ROOM = 2.0**15
FACTORS = 4
REACH = 28
GRANT = 24 << 20


def power_scale(largest):
    scale = jnp.ones_like(largest)
    factors = []
    for _ in range(FACTORS - 1):
        fits = largest * (scale * 2.0**REACH) < ROOM
        scale = jnp.where(fits, scale * 2.0**REACH, scale)
        factors.append(jnp.where(fits, ROOM * 2.0**-REACH, ROOM))
    last = jnp.full_like(largest, ROOM)
    for step in (16, 8, 4):
        fits = largest * (scale * 2.0**step) < ROOM
        scale = jnp.where(fits, scale * 2.0**step, scale)
        last = jnp.where(fits, last * 2.0**-step, last)
    factors.append(last)
    return scale, jnp.stack(factors, axis=1)


def fold_kernel(gain_in, up_in, down_in, out, gain, up, down, sems):
    loads = [
        pltpu.make_async_copy(source, target, sems.at[i])
        for i, (source, target) in enumerate(((gain_in, gain), (up_in, up), (down_in, down)))
    ]
    for load in loads:
        load.start()
    for load in loads:
        load.wait()
    chips, double, rows, _ = out.shape
    slabs = double // 2
    square = (rows, rows)
    here = lax.broadcasted_iota(jnp.int32, square, 0) == lax.broadcasted_iota(jnp.int32, square, 1)
    spread = jnp.sum(jnp.where(here, jnp.broadcast_to(gain[...], square), 0.0), axis=1, keepdims=True)
    for x in range(chips):
        for slab in range(slabs):
            first = (x * slabs + slab) * LANES
            out[x, slab] = (spread * up[:, first : first + LANES]).astype(jnp.bfloat16)
            out[x, slabs + slab] = down[:, first : first + LANES].astype(jnp.bfloat16)


def fold(gain, up, down, chips):
    rows, columns = up.shape
    slabs = columns // chips // LANES
    return pl.pallas_call(
        fold_kernel,
        out_shape=jax.ShapeDtypeStruct((chips, 2 * slabs, rows, LANES), jnp.bfloat16),
        in_specs=[pl.BlockSpec(memory_space=pl.ANY)] * 3,
        scratch_shapes=[
            pltpu.VMEM(gain.shape, jnp.float32),
            pltpu.VMEM(up.shape, jnp.float32),
            pltpu.VMEM(up.shape, jnp.float32),
            pltpu.SemaphoreType.DMA((3,)),
        ],
        cost_estimate=pl.CostEstimate(
            flops=2 * up.size, bytes_accessed=12 * up.size, transcendentals=0
        ),
    )(gain, up, down)


def norm_kernel(tokens, out, normed, sems):
    widened = tokens[...].astype(jnp.float32)
    mean = jnp.mean(widened * widened, axis=1, keepdims=True)
    normed[...] = (widened * lax.rsqrt(mean + 1e-06)).astype(jnp.bfloat16)
    copies = [pltpu.make_async_copy(normed, out.at[x], sems.at[x]) for x in range(out.shape[0])]
    for copy in copies:
        copy.start()
    for copy in copies:
        copy.wait()


def norm_copies(tokens, count):
    return pl.pallas_call(
        norm_kernel,
        out_shape=jax.ShapeDtypeStruct((count, *tokens.shape), jnp.bfloat16),
        out_specs=pl.BlockSpec(memory_space=pltpu.HBM),
        scratch_shapes=[
            pltpu.VMEM(tokens.shape, jnp.bfloat16),
            pltpu.SemaphoreType.DMA((count,)),
        ],
        cost_estimate=pl.CostEstimate(
            flops=2_000_000_000, bytes_accessed=10 * tokens.size, transcendentals=tokens.shape[0]
        ),
    )(tokens)


def apply_kernel(
    feat_rows, core_ref, tokens, weights, up_out, down_out, pieces, up, down, hidden, sems
):
    core = core_ref[0]
    x_count, rows, width = tokens.shape
    y_count = pieces.shape[0] // x_count
    part = width // y_count
    units = up_out.shape[1]
    z_count = weights.shape[0]
    feats = width // z_count
    slab_rows = x_count * feat_rows
    unit_slabs = units // LANES
    slabs = 2 * unit_slabs
    last = 2 * slabs * slab_rows

    def unpack(z, matrix, target):
        for source in range(2):
            first = last + matrix * FACTORS
            factors = weights[z, source, first : first + FACTORS].astype(jnp.float32)
            inverse = factors[0:1] * ROOM**-FACTORS
            for k in range(1, FACTORS):
                inverse = inverse * factors[k : k + 1]
            inverse = inverse.astype(jnp.bfloat16)
            for half in range(2):
                member = core if half == 0 else 1 - core
                for j in range(unit_slabs):
                    slab = matrix * slabs + member * unit_slabs + j
                    start = pl.multiple_of(slab * slab_rows, slab_rows)
                    values = weights[z, source, pl.ds(start, slab_rows)] * inverse
                    column = half * units + j * LANES
                    for x in range(x_count):
                        row = ((z * x_count + x) * 2 + source) * feat_rows
                        target[row : row + feat_rows, column : column + LANES] = values[
                            x * feat_rows : (x + 1) * feat_rows
                        ]

    copies = [
        pltpu.make_async_copy(source.at[:, :units], target, sems.at[i])
        for i, (source, target) in enumerate(((up, up_out), (down, down_out)))
    ]
    for first in range(0, z_count, 2):
        for z in range(first, first + 2):
            unpack(z, 0, up)
            unpack(z, 1, down)
        cols = slice(first * feats, (first + 2) * feats)
        term = jnp.dot(
            tokens[:, :, cols].reshape(x_count * rows, 2 * feats),
            up[cols, :],
            preferred_element_type=jnp.float32,
        )
        if first == 0:
            hidden[...] = term
        else:
            hidden[...] += term
    for copy in copies:
        copy.start()
    act = jnp.square(jnp.maximum(hidden[...], 0.0)).astype(jnp.bfloat16)
    for y in range(y_count):
        out = lax.dot_general(
            act,
            down[y * part : (y + 1) * part, :],
            (((1,), (1,)), ((), ())),
            preferred_element_type=jnp.float32,
        ).astype(jnp.bfloat16)
        for x in range(x_count):
            place = jnp.where(core == 0, x * y_count + y, y * x_count + x)
            pieces[place] = out[x * rows : (x + 1) * rows]
    for copy in copies:
        copy.wait()


def apply(core, tokens, weights, units, feat_rows, y_count):
    x_count, rows, width = tokens.shape
    weight = jax.ShapeDtypeStruct((width, units), jnp.bfloat16)
    vmem = pl.BlockSpec(memory_space=pltpu.VMEM)
    anywhere = pl.BlockSpec(memory_space=pl.ANY)
    return pl.pallas_call(
        functools.partial(apply_kernel, feat_rows),
        out_shape=(
            weight,
            weight,
            jax.ShapeDtypeStruct((x_count * y_count, rows, width // y_count), jnp.bfloat16),
        ),
        in_specs=[pl.BlockSpec(memory_space=pltpu.SMEM), vmem, vmem],
        out_specs=(anywhere, anywhere, vmem),
        scratch_shapes=[
            pltpu.VMEM((width, 2 * units), jnp.bfloat16),
            pltpu.VMEM((width, 2 * units), jnp.bfloat16),
            pltpu.VMEM((x_count * rows, 2 * units), jnp.float32),
            pltpu.SemaphoreType.DMA((2,)),
        ],
        cost_estimate=pl.CostEstimate(
            flops=8 * x_count * rows * width * units, bytes_accessed=16 << 20, transcendentals=0
        ),
        compiler_params=pltpu.CompilerParams(vmem_limit_bytes=GRANT),
    )(core, tokens, weights)


def crossed_groups(x_count, y_count):
    def at(x, c, y):
        return (x * 2 + c) * y_count + y

    def along_x(c):
        return [[at(x, c, y) for x in range(x_count)] for y in range(y_count)]

    def along_y(c):
        return [[at(x, c, y) for y in range(y_count)] for x in range(x_count)]

    return along_x(0) + along_y(1), along_y(0) + along_x(1)


def on_device(tokens, gain, up_master, down_master):
    feat_rows = up_master.shape[0]
    units = up_master.shape[1] // SUB
    x_count = lax.axis_size("x")
    y_count = lax.axis_size("y")
    both = fold(gain[None], up_master, down_master, x_count)
    both = lax.all_to_all(both, "x", 0, 0, tiled=True)
    gathered = lax.all_to_all(norm_copies(tokens, x_count), "x", 0, 0, tiled=True)

    block = both.astype(jnp.float32).reshape(x_count, 2, -1, feat_rows, LANES)
    scale, factors = power_scale(jnp.max(jnp.abs(block), axis=(0, 2, 3)))
    packed = (block * scale[None, :, None, None]).transpose(1, 2, 0, 3, 4).reshape(-1, LANES)
    packed = jnp.concatenate([packed, factors.reshape(-1, LANES)]).astype(jnp.float16)
    spread = lax.all_gather(packed[None], ("z", "c"), axis=0, tiled=True)
    spread, gathered = lax.optimization_barrier((spread, gathered))
    spread = spread.reshape(-1, 2, *packed.shape).astype(jnp.bfloat16)
    core = lax.axis_index("c").astype(jnp.int32)[None]
    up_own, down_own, pieces = apply(core, gathered, spread, units, feat_rows, y_count)
    for groups in crossed_groups(x_count, y_count):
        pieces = lax.all_to_all(
            pieces, ("x", "c", "y"), 0, 0, tiled=True, axis_index_groups=groups
        )
        pieces = pieces.reshape(len(groups[0]), -1, *pieces.shape[1:])
        pieces = jnp.sum(pieces.astype(jnp.float32), axis=0).astype(jnp.bfloat16)
    return up_own[None], down_own[None], pieces[0]


def solution(mesh):
    fine = Mesh(np.reshape(mesh.devices, (16, 4, 2, 4)), ("z", "x", "c", "y"))
    fs = ("z", "x", "c")
    return jax.shard_map(
        on_device,
        mesh=fine,
        in_specs=(P(fs, None), P(fs), P(fs, "y"), P(fs, "y")),
        out_specs=(P(fs, None, "y"), P(fs, None, "y"), P(fs, "y")),
        check_vma=False,
    )
```

```python
import functools

import jax
import jax.numpy as jnp
import numpy as np
from jax import lax
from jax.experimental import pallas as pl
from jax.experimental.pallas import tpu as pltpu
from jax.sharding import Mesh
from jax.sharding import PartitionSpec as P


SUB = 8
LANES = 128
ROOM = 2.0**15
FACTORS = 4
REACH = 28
GRANT = 24 << 20


def power_scale(largest):
    scale = jnp.ones_like(largest)
    factors = []
    for _ in range(FACTORS - 1):
        fits = largest * (scale * 2.0**REACH) < ROOM
        scale = jnp.where(fits, scale * 2.0**REACH, scale)
        factors.append(jnp.where(fits, ROOM * 2.0**-REACH, ROOM))
    last = jnp.full_like(largest, ROOM)
    for step in (16, 8, 4):
        fits = largest * (scale * 2.0**step) < ROOM
        scale = jnp.where(fits, scale * 2.0**step, scale)
        last = jnp.where(fits, last * 2.0**-step, last)
    factors.append(last)
    return scale, jnp.stack(factors, axis=1)


def prologue_kernel(x_ref, gain_in, up_in, down_in, tokens_in, *refs):
    blocks, (copies, gain, up, down, tokens, normed, sems) = refs[:-7], refs[-7:]
    chips = len(blocks)
    loads = [
        pltpu.make_async_copy(source, target, sems.at[i])
        for i, (source, target) in enumerate(
            ((tokens_in, tokens), (gain_in, gain), (up_in, up), (down_in, down))
        )
    ]
    for load in loads:
        load.start()
    loads[0].wait()
    widened = tokens[...].astype(jnp.float32)
    mean = jnp.mean(widened * widened, axis=1, keepdims=True)
    normed[...] = (widened * lax.rsqrt(mean + 1e-06)).astype(jnp.bfloat16)
    for load in loads[1:]:
        load.wait()
    stores = [
        pltpu.make_async_copy(normed, copies.at[i], sems.at[len(loads) + i]) for i in range(chips)
    ]
    for store in stores:
        store.start()
    double, rows, _ = blocks[0].shape
    slabs = double // 2
    square = (rows, rows)
    here = lax.broadcasted_iota(jnp.int32, square, 0) == lax.broadcasted_iota(jnp.int32, square, 1)
    spread = jnp.sum(jnp.where(here, jnp.broadcast_to(gain[...], square), 0.0), axis=1, keepdims=True)
    for ahead, block in enumerate(blocks):
        keeper = lax.rem(x_ref[0] + ahead, chips)
        for slab in range(slabs):
            at = pl.ds(pl.multiple_of((keeper * slabs + slab) * LANES, LANES), LANES)
            block[slab] = (spread * up[:, at]).astype(jnp.bfloat16)
            block[slabs + slab] = down[:, at].astype(jnp.bfloat16)
    for store in stores:
        store.wait()


def prologue(x, gain, up, down, tokens, chips):
    rows, columns = up.shape
    block = jax.ShapeDtypeStruct((2 * columns // chips // LANES, rows, LANES), jnp.bfloat16)
    anywhere = pl.BlockSpec(memory_space=pl.ANY)
    return pl.pallas_call(
        prologue_kernel,
        out_shape=(block,) * chips
        + (jax.ShapeDtypeStruct((chips, *tokens.shape), jnp.bfloat16),),
        in_specs=[pl.BlockSpec(memory_space=pltpu.SMEM)] + [anywhere] * 4,
        out_specs=(pl.BlockSpec(memory_space=pltpu.VMEM),) * chips + (anywhere,),
        scratch_shapes=[
            pltpu.VMEM(gain.shape, jnp.float32),
            pltpu.VMEM(up.shape, jnp.float32),
            pltpu.VMEM(up.shape, jnp.float32),
            pltpu.VMEM(tokens.shape, jnp.bfloat16),
            pltpu.VMEM(tokens.shape, jnp.bfloat16),
            pltpu.SemaphoreType.DMA((4 + chips,)),
        ],
        cost_estimate=pl.CostEstimate(
            flops=10 * tokens.size, bytes_accessed=10 * tokens.size, transcendentals=tokens.shape[0]
        ),
    )(x, gain, up, down, tokens)


def apply_kernel(
    feat_rows, place_ref, tokens, weights, up_out, down_out, pieces, up, down, hidden, sems
):
    core, chip = place_ref[0], place_ref[1]
    x_count, rows, width = tokens.shape
    y_count = pieces.shape[0] // x_count
    part = width // y_count
    units = up_out.shape[1]
    z_count = weights.shape[0]
    feats = width // z_count
    slab_rows = x_count * feat_rows
    unit_slabs = units // LANES
    slabs = 2 * unit_slabs
    last = 2 * slabs * slab_rows

    def unpack(z, matrix, target):
        for source in range(2):
            first = last + matrix * FACTORS
            factors = weights[z, source, first : first + FACTORS].astype(jnp.float32)
            inverse = factors[0:1] * ROOM**-FACTORS
            for k in range(1, FACTORS):
                inverse = inverse * factors[k : k + 1]
            inverse = inverse.astype(jnp.bfloat16)
            for half in range(2):
                member = core if half == 0 else 1 - core
                for j in range(unit_slabs):
                    slab = matrix * slabs + member * unit_slabs + j
                    start = pl.multiple_of(slab * slab_rows, slab_rows)
                    values = weights[z, source, pl.ds(start, slab_rows)] * inverse
                    column = half * units + j * LANES
                    for behind in range(x_count):
                        sender = lax.rem(chip + x_count - behind, x_count)
                        row = ((z * x_count + sender) * 2 + source) * feat_rows
                        target[
                            pl.ds(pl.multiple_of(row, feat_rows), feat_rows), column : column + LANES
                        ] = values[behind * feat_rows : (behind + 1) * feat_rows]

    copies = [
        pltpu.make_async_copy(source.at[:, :units], target, sems.at[i])
        for i, (source, target) in enumerate(((up, up_out), (down, down_out)))
    ]
    for first in range(0, z_count, 2):
        for z in range(first, first + 2):
            unpack(z, 0, up)
            unpack(z, 1, down)
        cols = slice(first * feats, (first + 2) * feats)
        term = jnp.dot(
            tokens[:, :, cols].reshape(x_count * rows, 2 * feats),
            up[cols, :],
            preferred_element_type=jnp.float32,
        )
        if first == 0:
            hidden[...] = term
        else:
            hidden[...] += term
    for copy in copies:
        copy.start()
    act = jnp.square(jnp.maximum(hidden[...], 0.0)).astype(jnp.bfloat16)
    for y in range(y_count):
        out = lax.dot_general(
            act,
            down[y * part : (y + 1) * part, :],
            (((1,), (1,)), ((), ())),
            preferred_element_type=jnp.float32,
        ).astype(jnp.bfloat16)
        for x in range(x_count):
            place = jnp.where(core == 0, x * y_count + y, y * x_count + x)
            pieces[place] = out[x * rows : (x + 1) * rows]
    for copy in copies:
        copy.wait()


def apply(place, tokens, weights, units, feat_rows, y_count):
    x_count, rows, width = tokens.shape
    weight = jax.ShapeDtypeStruct((width, units), jnp.bfloat16)
    vmem = pl.BlockSpec(memory_space=pltpu.VMEM)
    anywhere = pl.BlockSpec(memory_space=pl.ANY)
    return pl.pallas_call(
        functools.partial(apply_kernel, feat_rows),
        out_shape=(
            weight,
            weight,
            jax.ShapeDtypeStruct((x_count * y_count, rows, width // y_count), jnp.bfloat16),
        ),
        in_specs=[pl.BlockSpec(memory_space=pltpu.SMEM), vmem, vmem],
        out_specs=(anywhere, anywhere, vmem),
        scratch_shapes=[
            pltpu.VMEM((width, 2 * units), jnp.bfloat16),
            pltpu.VMEM((width, 2 * units), jnp.bfloat16),
            pltpu.VMEM((x_count * rows, 2 * units), jnp.float32),
            pltpu.SemaphoreType.DMA((2,)),
        ],
        cost_estimate=pl.CostEstimate(
            flops=8 * x_count * rows * width * units, bytes_accessed=16 << 20, transcendentals=0
        ),
        compiler_params=pltpu.CompilerParams(vmem_limit_bytes=GRANT),
    )(place, tokens, weights)


def crossed_groups(x_count, y_count):
    def at(x, c, y):
        return (x * 2 + c) * y_count + y

    def along_x(c):
        return [[at(x, c, y) for x in range(x_count)] for y in range(y_count)]

    def along_y(c):
        return [[at(x, c, y) for y in range(y_count)] for x in range(x_count)]

    return along_x(0) + along_y(1), along_y(0) + along_x(1)


def on_device(tokens, gain, up_master, down_master):
    feat_rows = up_master.shape[0]
    units = up_master.shape[1] // SUB
    x_count = lax.axis_size("x")
    y_count = lax.axis_size("y")
    chip = lax.axis_index("x").astype(jnp.int32)
    *blocks, copies = prologue(chip[None], gain[None], up_master, down_master, tokens, x_count)
    for ahead in range(1, x_count):
        blocks[ahead] = lax.ppermute(
            blocks[ahead], "x", [(i, (i + ahead) % x_count) for i in range(x_count)]
        )
    gathered = lax.all_to_all(copies, "x", 0, 0, tiled=True)

    block = jnp.stack(blocks).astype(jnp.float32).reshape(x_count, 2, -1, feat_rows, LANES)
    scale, factors = power_scale(jnp.max(jnp.abs(block), axis=(0, 2, 3)))
    packed = (block * scale[None, :, None, None]).transpose(1, 2, 0, 3, 4).reshape(-1, LANES)
    packed = jnp.concatenate([packed, factors.reshape(-1, LANES)]).astype(jnp.float16)
    spread = lax.all_gather(packed[None], ("z", "c"), axis=0, tiled=True)
    spread, gathered = lax.optimization_barrier((spread, gathered))
    spread = spread.reshape(-1, 2, *packed.shape).astype(jnp.bfloat16)
    place = jnp.stack([lax.axis_index("c").astype(jnp.int32), chip])
    up_own, down_own, pieces = apply(place, gathered, spread, units, feat_rows, y_count)
    for groups in crossed_groups(x_count, y_count):
        pieces = lax.all_to_all(
            pieces, ("x", "c", "y"), 0, 0, tiled=True, axis_index_groups=groups
        )
        pieces = pieces.reshape(len(groups[0]), -1, *pieces.shape[1:])
        pieces = jnp.sum(pieces.astype(jnp.float32), axis=0).astype(jnp.bfloat16)
    return up_own[None], down_own[None], pieces[0]


def solution(mesh):
    fine = Mesh(np.reshape(mesh.devices, (16, 4, 2, 4)), ("z", "x", "c", "y"))
    fs = ("z", "x", "c")
    return jax.shard_map(
        on_device,
        mesh=fine,
        in_specs=(P(fs, None), P(fs), P(fs, "y"), P(fs, "y")),
        out_specs=(P(fs, None, "y"), P(fs, None, "y"), P(fs, "y")),
        check_vma=False,
    )
```

```python
import functools

import jax
import jax.numpy as jnp
import numpy as np
from jax import lax
from jax.experimental import pallas as pl
from jax.experimental.pallas import tpu as pltpu
from jax.sharding import Mesh
from jax.sharding import PartitionSpec as P


SUB = 8
LANES = 128
ROOM = 2.0**15
FACTORS = 4
REACH = 28
GRANT = 24 << 20


def power_scale(largest):
    scale = jnp.ones_like(largest)
    factors = []
    for _ in range(FACTORS - 1):
        fits = largest * (scale * 2.0**REACH) < ROOM
        scale = jnp.where(fits, scale * 2.0**REACH, scale)
        factors.append(jnp.where(fits, ROOM * 2.0**-REACH, ROOM))
    last = jnp.full_like(largest, ROOM)
    for step in (16, 8, 4):
        fits = largest * (scale * 2.0**step) < ROOM
        scale = jnp.where(fits, scale * 2.0**step, scale)
        last = jnp.where(fits, last * 2.0**-step, last)
    factors.append(last)
    return scale, jnp.stack(factors, axis=1)


def fold_kernel(gain_in, up_in, down_in, out, gain, up, down, sems):
    loads = [
        pltpu.make_async_copy(source, target, sems.at[i])
        for i, (source, target) in enumerate(((gain_in, gain), (up_in, up), (down_in, down)))
    ]
    for load in loads:
        load.start()
    for load in loads:
        load.wait()
    chips, double, rows, _ = out.shape
    slabs = double // 2
    square = (rows, rows)
    here = lax.broadcasted_iota(jnp.int32, square, 0) == lax.broadcasted_iota(jnp.int32, square, 1)
    spread = jnp.sum(jnp.where(here, jnp.broadcast_to(gain[...], square), 0.0), axis=1, keepdims=True)
    for x in range(chips):
        for slab in range(slabs):
            first = (x * slabs + slab) * LANES
            out[x, slab] = (spread * up[:, first : first + LANES]).astype(jnp.bfloat16)
            out[x, slabs + slab] = down[:, first : first + LANES].astype(jnp.bfloat16)


def fold(gain, up, down, chips):
    rows, columns = up.shape
    slabs = columns // chips // LANES
    return pl.pallas_call(
        fold_kernel,
        out_shape=jax.ShapeDtypeStruct((chips, 2 * slabs, rows, LANES), jnp.bfloat16),
        in_specs=[pl.BlockSpec(memory_space=pl.ANY)] * 3,
        scratch_shapes=[
            pltpu.VMEM(gain.shape, jnp.float32),
            pltpu.VMEM(up.shape, jnp.float32),
            pltpu.VMEM(up.shape, jnp.float32),
            pltpu.SemaphoreType.DMA((3,)),
        ],
        cost_estimate=pl.CostEstimate(
            flops=2 * up.size, bytes_accessed=12 * up.size, transcendentals=0
        ),
    )(gain, up, down)


def norm_factor(tokens):
    widened = tokens.astype(jnp.float32)
    return lax.rsqrt(jnp.mean(widened * widened, axis=1, keepdims=True) + 1e-06)


def apply_kernel(
    feat_rows, place_ref, *refs
):
    *tokens, weights, up_out, down_out, pieces, up, down, hidden, sems = refs
    core, chip = place_ref[0], place_ref[1]
    x_count = len(tokens)
    rows, width = tokens[0].shape
    y_count = pieces.shape[0] // x_count
    part = width // y_count
    units = up_out.shape[1]
    z_count = weights.shape[0]
    feats = width // z_count
    slab_rows = x_count * feat_rows
    unit_slabs = units // LANES
    slabs = 2 * unit_slabs
    last = 2 * slabs * slab_rows

    def unpack(z, matrix, target):
        for source in range(2):
            first = last + matrix * FACTORS
            factors = weights[z, source, first : first + FACTORS].astype(jnp.float32)
            inverse = factors[0:1] * ROOM**-FACTORS
            for k in range(1, FACTORS):
                inverse = inverse * factors[k : k + 1]
            inverse = inverse.astype(jnp.bfloat16)
            for half in range(2):
                member = core if half == 0 else 1 - core
                for j in range(unit_slabs):
                    slab = matrix * slabs + member * unit_slabs + j
                    start = pl.multiple_of(slab * slab_rows, slab_rows)
                    values = weights[z, source, pl.ds(start, slab_rows)] * inverse
                    column = half * units + j * LANES
                    for x in range(x_count):
                        row = ((z * x_count + x) * 2 + source) * feat_rows
                        target[row : row + feat_rows, column : column + LANES] = values[
                            x * feat_rows : (x + 1) * feat_rows
                        ]

    copies = [
        pltpu.make_async_copy(source.at[:, :units], target, sems.at[i])
        for i, (source, target) in enumerate(((up, up_out), (down, down_out)))
    ]
    for first in range(0, z_count, 2):
        for z in range(first, first + 2):
            unpack(z, 0, up)
            unpack(z, 1, down)
        cols = slice(first * feats, (first + 2) * feats)
        term = jnp.dot(
            jnp.concatenate([block[:, cols] for block in tokens]),
            up[cols, :],
            preferred_element_type=jnp.float32,
        )
        if first == 0:
            hidden[...] = term
        else:
            hidden[...] += term
    for copy in copies:
        copy.start()
    factor = jnp.concatenate([norm_factor(block[...]) for block in tokens])
    act = jnp.square(jnp.maximum(hidden[...] * factor, 0.0)).astype(jnp.bfloat16)
    for y in range(y_count):
        out = lax.dot_general(
            act,
            down[y * part : (y + 1) * part, :],
            (((1,), (1,)), ((), ())),
            preferred_element_type=jnp.float32,
        ).astype(jnp.bfloat16)
        for ahead in range(x_count):
            x = lax.rem(chip + ahead, x_count)
            place = jnp.where(core == 0, x * y_count + y, y * x_count + x)
            pieces[place] = out[ahead * rows : (ahead + 1) * rows]
    for copy in copies:
        copy.wait()


def apply(place, tokens, weights, units, feat_rows, y_count):
    x_count = len(tokens)
    rows, width = tokens[0].shape
    weight = jax.ShapeDtypeStruct((width, units), jnp.bfloat16)
    vmem = pl.BlockSpec(memory_space=pltpu.VMEM)
    anywhere = pl.BlockSpec(memory_space=pl.ANY)
    return pl.pallas_call(
        functools.partial(apply_kernel, feat_rows),
        out_shape=(
            weight,
            weight,
            jax.ShapeDtypeStruct((x_count * y_count, rows, width // y_count), jnp.bfloat16),
        ),
        in_specs=[pl.BlockSpec(memory_space=pltpu.SMEM)] + [vmem] * (x_count + 1),
        out_specs=(anywhere, anywhere, vmem),
        scratch_shapes=[
            pltpu.VMEM((width, 2 * units), jnp.bfloat16),
            pltpu.VMEM((width, 2 * units), jnp.bfloat16),
            pltpu.VMEM((x_count * rows, 2 * units), jnp.float32),
            pltpu.SemaphoreType.DMA((2,)),
        ],
        cost_estimate=pl.CostEstimate(
            flops=8 * x_count * rows * width * units, bytes_accessed=16 << 20, transcendentals=0
        ),
        compiler_params=pltpu.CompilerParams(vmem_limit_bytes=GRANT),
    )(place, *tokens, weights)


def crossed_groups(x_count, y_count):
    def at(x, c, y):
        return (x * 2 + c) * y_count + y

    def along_x(c):
        return [[at(x, c, y) for x in range(x_count)] for y in range(y_count)]

    def along_y(c):
        return [[at(x, c, y) for y in range(y_count)] for x in range(x_count)]

    return along_x(0) + along_y(1), along_y(0) + along_x(1)


def on_device(tokens, gain, up_master, down_master):
    feat_rows = up_master.shape[0]
    units = up_master.shape[1] // SUB
    x_count = lax.axis_size("x")
    y_count = lax.axis_size("y")
    both = fold(gain[None], up_master, down_master, x_count)
    held = [tokens]
    both = lax.all_to_all(both, "x", 0, 0, tiled=True)
    for ahead in range(1, x_count):
        held.append(lax.ppermute(tokens, "x", [((i + ahead) % x_count, i) for i in range(x_count)]))

    block = both.astype(jnp.float32).reshape(x_count, 2, -1, feat_rows, LANES)
    scale, factors = power_scale(jnp.max(jnp.abs(block), axis=(0, 2, 3)))
    packed = (block * scale[None, :, None, None]).transpose(1, 2, 0, 3, 4).reshape(-1, LANES)
    packed = jnp.concatenate([packed, factors.reshape(-1, LANES)]).astype(jnp.float16)
    spread = lax.all_gather(packed[None], ("z", "c"), axis=0, tiled=True)
    spread = spread.reshape(-1, 2, *packed.shape).astype(jnp.bfloat16)
    place = jnp.stack([lax.axis_index(axis).astype(jnp.int32) for axis in ("c", "x")])
    up_own, down_own, pieces = apply(place, held, spread, units, feat_rows, y_count)
    for groups in crossed_groups(x_count, y_count):
        pieces = lax.all_to_all(
            pieces, ("x", "c", "y"), 0, 0, tiled=True, axis_index_groups=groups
        )
        pieces = pieces.reshape(len(groups[0]), -1, *pieces.shape[1:])
        pieces = jnp.sum(pieces.astype(jnp.float32), axis=0).astype(jnp.bfloat16)
    return up_own[None], down_own[None], pieces[0]


def solution(mesh):
    fine = Mesh(np.reshape(mesh.devices, (16, 4, 2, 4)), ("z", "x", "c", "y"))
    fs = ("z", "x", "c")
    return jax.shard_map(
        on_device,
        mesh=fine,
        in_specs=(P(fs, None), P(fs), P(fs, "y"), P(fs, "y")),
        out_specs=(P(fs, None, "y"), P(fs, None, "y"), P(fs, "y")),
        check_vma=False,
    )
```

```python
import functools

import jax
import jax.numpy as jnp
import numpy as np
from jax import lax
from jax.experimental import pallas as pl
from jax.experimental.pallas import tpu as pltpu
from jax.sharding import Mesh
from jax.sharding import PartitionSpec as P


SUB = 8
LANES = 128
ROOM = 2.0**15
FACTORS = 4
REACH = 28
GRANT = 24 << 20


def power_scale(largest):
    scale = jnp.ones_like(largest)
    factors = []
    for _ in range(FACTORS - 1):
        fits = largest * (scale * 2.0**REACH) < ROOM
        scale = jnp.where(fits, scale * 2.0**REACH, scale)
        factors.append(jnp.where(fits, ROOM * 2.0**-REACH, ROOM))
    last = jnp.full_like(largest, ROOM)
    for step in (16, 8, 4):
        fits = largest * (scale * 2.0**step) < ROOM
        scale = jnp.where(fits, scale * 2.0**step, scale)
        last = jnp.where(fits, last * 2.0**-step, last)
    factors.append(last)
    return scale, jnp.stack(factors, axis=1)


def fold_kernel(gain_in, up_in, down_in, out, gain, up, down, sems):
    loads = [
        pltpu.make_async_copy(source, target, sems.at[i])
        for i, (source, target) in enumerate(((gain_in, gain), (up_in, up), (down_in, down)))
    ]
    for load in loads:
        load.start()
    for load in loads:
        load.wait()
    chips, double, rows, _ = out.shape
    slabs = double // 2
    square = (rows, rows)
    here = lax.broadcasted_iota(jnp.int32, square, 0) == lax.broadcasted_iota(jnp.int32, square, 1)
    spread = jnp.sum(jnp.where(here, jnp.broadcast_to(gain[...], square), 0.0), axis=1, keepdims=True)
    for x in range(chips):
        for slab in range(slabs):
            first = (x * slabs + slab) * LANES
            out[x, slab] = (spread * up[:, first : first + LANES]).astype(jnp.bfloat16)
            out[x, slabs + slab] = down[:, first : first + LANES].astype(jnp.bfloat16)


def fold(gain, up, down, chips):
    rows, columns = up.shape
    slabs = columns // chips // LANES
    return pl.pallas_call(
        fold_kernel,
        out_shape=jax.ShapeDtypeStruct((chips, 2 * slabs, rows, LANES), jnp.bfloat16),
        in_specs=[pl.BlockSpec(memory_space=pl.ANY)] * 3,
        scratch_shapes=[
            pltpu.VMEM(gain.shape, jnp.float32),
            pltpu.VMEM(up.shape, jnp.float32),
            pltpu.VMEM(up.shape, jnp.float32),
            pltpu.SemaphoreType.DMA((3,)),
        ],
        cost_estimate=pl.CostEstimate(
            flops=2 * up.size, bytes_accessed=12 * up.size, transcendentals=0
        ),
    )(gain, up, down)


def apply_kernel(
    feat_rows, place_ref, *refs
):
    *tokens, weights, up_out, down_out, pieces, up, up_other, down, down_other, hidden, squares, sems = refs
    core, chip = place_ref[0], place_ref[1]
    x_count = len(tokens)
    rows, width = tokens[0].shape
    y_count = pieces.shape[0] // x_count
    part = width // y_count
    units = up_out.shape[1]
    z_count = weights.shape[0]
    feats = width // z_count
    slab_rows = x_count * feat_rows
    unit_slabs = units // LANES
    slabs = 2 * unit_slabs
    last = 2 * slabs * slab_rows

    def unpack(z, matrix, targets):
        for source in range(2):
            first = last + matrix * FACTORS
            factors = weights[z, source, first : first + FACTORS].astype(jnp.float32)
            inverse = factors[0:1] * ROOM**-FACTORS
            for k in range(1, FACTORS):
                inverse = inverse * factors[k : k + 1]
            inverse = inverse.astype(jnp.bfloat16)
            for half in range(2):
                member = core if half == 0 else 1 - core
                for j in range(unit_slabs):
                    slab = matrix * slabs + member * unit_slabs + j
                    start = pl.multiple_of(slab * slab_rows, slab_rows)
                    values = weights[z, source, pl.ds(start, slab_rows)] * inverse
                    column, target = j * LANES, targets[half]
                    for x in range(x_count):
                        row = ((z * x_count + x) * 2 + source) * feat_rows
                        target[row : row + feat_rows, column : column + LANES] = values[
                            x * feat_rows : (x + 1) * feat_rows
                        ]

    copies = []
    for first in range(0, z_count, 2):
        for z in range(first, first + 2):
            unpack(z, 0, (up, up_other))
            unpack(z, 1, (down, down_other))
        if first % 4 == 2:
            part_rows = slice((first - 2) * feats, (first + 2) * feats)
            for source, target in ((up, up_out), (down, down_out)):
                copies.append(
                    pltpu.make_async_copy(
                        source.at[part_rows], target.at[part_rows], sems.at[len(copies)]
                    )
                )
        cols = slice(first * feats, (first + 2) * feats)
        for ahead, block in enumerate(tokens):
            widened = block[:, cols].astype(jnp.float32)
            term = sum(
                jnp.square(widened[:, i : i + LANES]) for i in range(0, 2 * feats, LANES)
            )
            at = slice(ahead * rows, (ahead + 1) * rows)
            if first == 0:
                squares[at] = term
            else:
                squares[at] += term
        joined = jnp.concatenate([block[:, cols] for block in tokens])
        for half, weight in enumerate((up, up_other)):
            at = slice(half * units, (half + 1) * units)
            term = jnp.dot(joined, weight[cols, :], preferred_element_type=jnp.float32)
            if first == 0:
                hidden[:, at] = term
            else:
                hidden[:, at] += term
        if first % 4 == 2:
            for copy in copies[-2:]:
                copy.start()
    factor = lax.rsqrt(jnp.sum(squares[...], axis=1, keepdims=True) / width + 1e-06)
    act = jnp.square(jnp.maximum(hidden[...] * factor, 0.0)).astype(jnp.bfloat16)
    for y in range(y_count):
        out = sum(
            lax.dot_general(
                act[:, half * units : (half + 1) * units],
                weight[y * part : (y + 1) * part, :],
                (((1,), (1,)), ((), ())),
                preferred_element_type=jnp.float32,
            )
            for half, weight in enumerate((down, down_other))
        ).astype(jnp.bfloat16)
        for ahead in range(x_count):
            x = lax.rem(chip + ahead, x_count)
            place = jnp.where(core == 1, x * y_count + y, y * x_count + x)
            pieces[place] = out[ahead * rows : (ahead + 1) * rows]
    for copy in copies:
        copy.wait()


def apply(place, tokens, weights, units, feat_rows, y_count):
    x_count = len(tokens)
    rows, width = tokens[0].shape
    weight = jax.ShapeDtypeStruct((width, units), jnp.bfloat16)
    vmem = pl.BlockSpec(memory_space=pltpu.VMEM)
    anywhere = pl.BlockSpec(memory_space=pl.ANY)
    return pl.pallas_call(
        functools.partial(apply_kernel, feat_rows),
        out_shape=(
            weight,
            weight,
            jax.ShapeDtypeStruct((x_count * y_count, rows, width // y_count), jnp.bfloat16),
        ),
        in_specs=[pl.BlockSpec(memory_space=pltpu.SMEM)] + [vmem] * (x_count + 1),
        out_specs=(anywhere, anywhere, vmem),
        scratch_shapes=[
            pltpu.VMEM((width, units), jnp.bfloat16),
            pltpu.VMEM((width, units), jnp.bfloat16),
            pltpu.VMEM((width, units), jnp.bfloat16),
            pltpu.VMEM((width, units), jnp.bfloat16),
            pltpu.VMEM((x_count * rows, 2 * units), jnp.float32),
            pltpu.VMEM((x_count * rows, LANES), jnp.float32),
            pltpu.SemaphoreType.DMA((weights.shape[0] // 2,)),
        ],
        cost_estimate=pl.CostEstimate(
            flops=8 * x_count * rows * width * units, bytes_accessed=16 << 20, transcendentals=0
        ),
        compiler_params=pltpu.CompilerParams(vmem_limit_bytes=GRANT),
    )(place, *tokens, weights)


def crossed_groups(x_count, y_count):
    def at(x, c, y):
        return (x * 2 + c) * y_count + y

    def along_x(c):
        return [[at(x, c, y) for x in range(x_count)] for y in range(y_count)]

    def along_y(c):
        return [[at(x, c, y) for y in range(y_count)] for x in range(x_count)]

    return along_x(1) + along_y(0), along_y(1) + along_x(0)


def on_device(tokens, gain, up_master, down_master):
    feat_rows = up_master.shape[0]
    units = up_master.shape[1] // SUB
    x_count = lax.axis_size("x")
    y_count = lax.axis_size("y")
    both = fold(gain[None], up_master, down_master, x_count)
    held = [tokens]
    both = lax.all_to_all(both, "x", 0, 0, tiled=True)
    for ahead in range(1, x_count):
        held.append(
            lax.ppermute(tokens, "x", [((i + ahead) % x_count, i) for i in range(x_count)])
        )

    block = both.astype(jnp.float32).reshape(x_count, 2, -1, feat_rows, LANES)
    scale, factors = power_scale(jnp.max(jnp.abs(block), axis=(0, 2, 3)))
    packed = (block * scale[None, :, None, None]).transpose(1, 2, 0, 3, 4).reshape(-1, LANES)
    packed = jnp.concatenate([packed, factors.reshape(-1, LANES)]).astype(jnp.float16)
    spread = lax.all_gather(packed[None], ("z", "c"), axis=0, tiled=True)
    spread = spread.reshape(-1, 2, *packed.shape).astype(jnp.bfloat16)
    place = jnp.stack([lax.axis_index(axis).astype(jnp.int32) for axis in ("c", "x")])
    up_own, down_own, pieces = apply(place, held, spread, units, feat_rows, y_count)
    for groups in crossed_groups(x_count, y_count):
        pieces = lax.all_to_all(
            pieces, ("x", "c", "y"), 0, 0, tiled=True, axis_index_groups=groups
        )
        pieces = pieces.reshape(len(groups[0]), -1, *pieces.shape[1:])
        pieces = jnp.sum(pieces.astype(jnp.float32), axis=0).astype(jnp.bfloat16)
    return up_own[None], down_own[None], pieces[0]


def solution(mesh):
    fine = Mesh(np.reshape(mesh.devices, (16, 4, 2, 4)), ("z", "x", "c", "y"))
    fs = ("z", "x", "c")
    return jax.shard_map(
        on_device,
        mesh=fine,
        in_specs=(P(fs, None), P(fs), P(fs, "y"), P(fs, "y")),
        out_specs=(P(fs, None, "y"), P(fs, None, "y"), P(fs, "y")),
        check_vma=False,
    )
```

```python
import functools

import jax
import jax.numpy as jnp
import numpy as np
from jax import lax
from jax.experimental import pallas as pl
from jax.experimental.pallas import tpu as pltpu
from jax.sharding import Mesh
from jax.sharding import PartitionSpec as P


SUB = 8
LANES = 128
ROOM = 2.0**15
FACTORS = 4
REACH = 28
GRANT = 24 << 20


def power_scale(largest):
    scale = jnp.ones_like(largest)
    factors = []
    for _ in range(FACTORS - 1):
        fits = largest * (scale * 2.0**REACH) < ROOM
        scale = jnp.where(fits, scale * 2.0**REACH, scale)
        factors.append(jnp.where(fits, ROOM * 2.0**-REACH, ROOM))
    last = jnp.full_like(largest, ROOM)
    for step in (16, 8, 4):
        fits = largest * (scale * 2.0**step) < ROOM
        scale = jnp.where(fits, scale * 2.0**step, scale)
        last = jnp.where(fits, last * 2.0**-step, last)
    factors.append(last)
    return scale, jnp.stack(factors, axis=1)


def fold_kernel(gain_in, up_in, down_in, out, gain, up, down, sems):
    loads = [
        pltpu.make_async_copy(source, target, sems.at[i])
        for i, (source, target) in enumerate(((gain_in, gain), (up_in, up), (down_in, down)))
    ]
    for load in loads:
        load.start()
    for load in loads:
        load.wait()
    chips, double, rows, _ = out.shape
    slabs = double // 2
    square = (rows, rows)
    here = lax.broadcasted_iota(jnp.int32, square, 0) == lax.broadcasted_iota(jnp.int32, square, 1)
    spread = jnp.sum(jnp.where(here, jnp.broadcast_to(gain[...], square), 0.0), axis=1, keepdims=True)
    for x in range(chips):
        for slab in range(slabs):
            first = (x * slabs + slab) * LANES
            out[x, slab] = (spread * up[:, first : first + LANES]).astype(jnp.bfloat16)
            out[x, slabs + slab] = down[:, first : first + LANES].astype(jnp.bfloat16)


def fold(gain, up, down, chips):
    rows, columns = up.shape
    slabs = columns // chips // LANES
    return pl.pallas_call(
        fold_kernel,
        out_shape=jax.ShapeDtypeStruct((chips, 2 * slabs, rows, LANES), jnp.bfloat16),
        in_specs=[pl.BlockSpec(memory_space=pl.ANY)] * 3,
        scratch_shapes=[
            pltpu.VMEM(gain.shape, jnp.float32),
            pltpu.VMEM(up.shape, jnp.float32),
            pltpu.VMEM(up.shape, jnp.float32),
            pltpu.SemaphoreType.DMA((3,)),
        ],
        cost_estimate=pl.CostEstimate(
            flops=2 * up.size, bytes_accessed=12 * up.size, transcendentals=0
        ),
    )(gain, up, down)


def apply_kernel(
    feat_rows, place_ref, *refs
):
    *tokens, weights, up_out, down_out, pieces, up, down, hidden, squares, sems = refs
    core, chip = place_ref[0], place_ref[1]
    x_count = len(tokens)
    rows, width = tokens[0].shape
    y_count = pieces.shape[0] // x_count
    part = width // y_count
    units = up_out.shape[1]
    z_count = weights.shape[0]
    feats = width // z_count
    slab_rows = x_count * feat_rows
    unit_slabs = units // LANES
    slabs = 2 * unit_slabs
    last = 2 * slabs * slab_rows

    def unpack(z, matrix, target):
        for source in range(2):
            first = last + matrix * FACTORS
            factors = weights[z, source, first : first + FACTORS].astype(jnp.float32)
            inverse = factors[0:1] * ROOM**-FACTORS
            for k in range(1, FACTORS):
                inverse = inverse * factors[k : k + 1]
            inverse = inverse.astype(jnp.bfloat16)
            for half in range(2):
                member = core if half == 0 else 1 - core
                for j in range(unit_slabs):
                    slab = matrix * slabs + member * unit_slabs + j
                    start = pl.multiple_of(slab * slab_rows, slab_rows)
                    values = weights[z, source, pl.ds(start, slab_rows)] * inverse
                    column = half * units + j * LANES
                    for x in range(x_count):
                        row = ((z * x_count + x) * 2 + source) * feat_rows
                        target[row : row + feat_rows, column : column + LANES] = values[
                            x * feat_rows : (x + 1) * feat_rows
                        ]

    copies = []
    for first in range(0, z_count, 2):
        for z in range(first, first + 2):
            unpack(z, 0, up)
            unpack(z, 1, down)
        if first % 4 == 2:
            part_rows = slice((first - 2) * feats, (first + 2) * feats)
            for source, target in ((up, up_out), (down, down_out)):
                copies.append(
                    pltpu.make_async_copy(
                        source.at[part_rows, :units], target.at[part_rows, :], sems.at[len(copies)]
                    )
                )
        cols = slice(first * feats, (first + 2) * feats)
        for ahead, block in enumerate(tokens):
            widened = block[:, cols].astype(jnp.float32)
            term = sum(
                jnp.square(widened[:, i : i + LANES]) for i in range(0, 2 * feats, LANES)
            )
            at = slice(ahead * rows, (ahead + 1) * rows)
            if first == 0:
                squares[at] = term
            else:
                squares[at] += term
        term = jnp.dot(
            jnp.concatenate([block[:, cols] for block in tokens]),
            up[cols, :],
            preferred_element_type=jnp.float32,
        )
        if first == 0:
            hidden[...] = term
        else:
            hidden[...] += term
        if first % 4 == 2:
            for copy in copies[-2:]:
                copy.start()
    factor = lax.rsqrt(jnp.sum(squares[...], axis=1, keepdims=True) / width + 1e-06)
    act = jnp.square(jnp.maximum(hidden[...] * factor, 0.0)).astype(jnp.bfloat16)
    for y in range(y_count):
        out = lax.dot_general(
            act,
            down[y * part : (y + 1) * part, :],
            (((1,), (1,)), ((), ())),
            preferred_element_type=jnp.float32,
        ).astype(jnp.bfloat16)
        for ahead in range(x_count):
            x = lax.rem(chip + ahead, x_count)
            place = jnp.where(core == 1, x * y_count + y, y * x_count + x)
            pieces[place] = out[ahead * rows : (ahead + 1) * rows]
    for copy in copies:
        copy.wait()


def apply(place, tokens, weights, units, feat_rows, y_count):
    x_count = len(tokens)
    rows, width = tokens[0].shape
    weight = jax.ShapeDtypeStruct((width, units), jnp.bfloat16)
    vmem = pl.BlockSpec(memory_space=pltpu.VMEM)
    anywhere = pl.BlockSpec(memory_space=pl.ANY)
    return pl.pallas_call(
        functools.partial(apply_kernel, feat_rows),
        out_shape=(
            weight,
            weight,
            jax.ShapeDtypeStruct((x_count * y_count, rows, width // y_count), jnp.bfloat16),
        ),
        in_specs=[pl.BlockSpec(memory_space=pltpu.SMEM)] + [vmem] * (x_count + 1),
        out_specs=(anywhere, anywhere, vmem),
        scratch_shapes=[
            pltpu.VMEM((width, 2 * units), jnp.bfloat16),
            pltpu.VMEM((width, 2 * units), jnp.bfloat16),
            pltpu.VMEM((x_count * rows, 2 * units), jnp.float32),
            pltpu.VMEM((x_count * rows, LANES), jnp.float32),
            pltpu.SemaphoreType.DMA((weights.shape[0] // 2,)),
        ],
        cost_estimate=pl.CostEstimate(
            flops=8 * x_count * rows * width * units, bytes_accessed=16 << 20, transcendentals=0
        ),
        compiler_params=pltpu.CompilerParams(vmem_limit_bytes=GRANT),
    )(place, *tokens, weights)


def crossed_groups(x_count, y_count):
    def at(x, c, y):
        return (x * 2 + c) * y_count + y

    def along_x(c):
        return [[at(x, c, y) for x in range(x_count)] for y in range(y_count)]

    def along_y(c):
        return [[at(x, c, y) for y in range(y_count)] for x in range(x_count)]

    return along_x(1) + along_y(0), along_y(1) + along_x(0)


def on_device(tokens, gain, up_master, down_master):
    feat_rows = up_master.shape[0]
    units = up_master.shape[1] // SUB
    x_count = lax.axis_size("x")
    y_count = lax.axis_size("y")
    both = fold(gain[None], up_master, down_master, x_count)
    held = [tokens]
    both = lax.all_to_all(both, "x", 0, 0, tiled=True)
    for ahead in range(1, x_count):
        held.append(lax.ppermute(tokens, "x", [((i + ahead) % x_count, i) for i in range(x_count)]))

    block = both.astype(jnp.float32).reshape(x_count, 2, -1, feat_rows, LANES)
    scale, factors = power_scale(jnp.max(jnp.abs(block), axis=(0, 2, 3)))
    packed = (block * scale[None, :, None, None]).transpose(1, 2, 0, 3, 4).reshape(-1, LANES)
    packed = jnp.concatenate([packed, factors.reshape(-1, LANES)]).astype(jnp.float16)
    spread = lax.all_gather(packed[None], ("z", "c"), axis=0, tiled=True)
    spread = spread.reshape(-1, 2, *packed.shape).astype(jnp.bfloat16)
    place = jnp.stack([lax.axis_index(axis).astype(jnp.int32) for axis in ("c", "x")])
    up_own, down_own, pieces = apply(place, held, spread, units, feat_rows, y_count)
    for groups in crossed_groups(x_count, y_count):
        pieces = lax.all_to_all(
            pieces, ("x", "c", "y"), 0, 0, tiled=True, axis_index_groups=groups
        )
        pieces = pieces.reshape(len(groups[0]), -1, *pieces.shape[1:])
        pieces = jnp.sum(pieces.astype(jnp.float32), axis=0).astype(jnp.bfloat16)
    return up_own[None], down_own[None], pieces[0]


def solution(mesh):
    fine = Mesh(np.reshape(mesh.devices, (16, 4, 2, 4)), ("z", "x", "c", "y"))
    fs = ("z", "x", "c")
    return jax.shard_map(
        on_device,
        mesh=fine,
        in_specs=(P(fs, None), P(fs), P(fs, "y"), P(fs, "y")),
        out_specs=(P(fs, None, "y"), P(fs, None, "y"), P(fs, "y")),
        check_vma=False,
    )
```
